32 devices in a mesh: tp: 32 (over z, y, x, core).
Axes of the slice: x: 2, y: 2, z: 4, core: 2. Of those that a mesh axis runs over, the one named last changes fastest.
Arguments:
- tokens: bfloat16 [32, 4096], replicated, may hold values from -18 to 18
- norm_gain: float32 [2, 4096], replicated, may hold values from 0.1 to 1.9
- w_gate: bfloat16 [2, 4096, 8192], P(None, None, 'tp'), may hold values from -0.09375 to 0.09375
- w_value: bfloat16 [2, 4096, 8192], P(None, None, 'tp'), may hold values from -0.09375 to 0.09375
- w_write: bfloat16 [2, 4096, 1024], P(None, None, 'tp'), may hold values from -0.09375 to 0.09375
- w_read: bfloat16 [2, 4096, 1024], P(None, None, 'tp'), may hold values from -0.09375 to 0.09375
- w_step: bfloat16 [2, 4096, 128], replicated, may hold values from -0.09375 to 0.09375
- step_bias: float32 [2, 128], replicated, may hold values from -2 to 1
- decay_rate: float32 [2, 128], replicated, may hold values from 0.05 to 3
- skip_gain: float32 [2, 128], replicated, may hold values from 1 to 4
- conv_value_weight: float32 [2, 3, 8192], P(None, None, 'tp'), may hold values from -2.5 to 2.5
- conv_key_weight: float32 [2, 3, 2, 1024], P(None, None, None, 'tp'), may hold values from -2.5 to 2.5
- group_gain: float32 [2, 8192], P(None, 'tp'), may hold values from 0.1 to 1.9
- w_out: bfloat16 [2, 8192, 4096], P(None, 'tp'), may hold values from -0.0625 to 0.0625
- ssm_state: float32 [2, 32, 8192, 128], P(None, None, 'tp'), may hold values from -3 to 3
- conv_value: float32 [2, 32, 2, 8192], P(None, None, None, 'tp'), may hold values from -5 to 5
- conv_key: float32 [2, 32, 2, 2, 1024], P(None, None, None, None, 'tp'), may hold values from -5 to 5
Outputs:
- tokens_out: bfloat16 [32, 4096], replicated
- ssm_state_out: float32 [2, 32, 8192, 128], P(None, None, 'tp')
- conv_value_out: float32 [2, 32, 2, 8192], P(None, None, None, 'tp')
- conv_key_out: float32 [2, 32, 2, 2, 1024], P(None, None, None, None, 'tp')
The draws below stay inside these ranges and needn't reach their ends.
All inputs are finite; a program needn't handle non-finite values.
Results may differ from the reference program's by a relative error of at most 0.011.
Values may be sent and summed in bfloat16 or wider, within the bound.
A program may use at most 128 MiB of HBM per device.

```python
import math
import jax
import jax.numpy as jnp
from jax import lax

D = 4096
SSDW = 8192
HEAD_DIM = 64
GROUPS = 8
STATE = 128
CONV = 3
LAYERS = 2
BATCH = 32
HEADS = 128
HPG = 16
GW = 1024


def draw_tokens(key, part):
    key_scale, key_value = jax.random.split(key)
    column_scale = jnp.exp(jax.random.uniform(key_scale, (1, D), jnp.float32, math.log(0.3), math.log(3.0)))
    values = jnp.clip(jax.random.normal(key_value, (BATCH, D), jnp.float32), -6.0, 6.0)
    return (values * column_scale).astype(jnp.bfloat16)


def levels(stream_key, dims, cuts, smallest, high):
    gain, own = 1.0, jax.random.fold_in(stream_key, 6)
    for axis_at, shards_of in cuts:
        heights = jnp.exp(jax.random.uniform(jax.random.fold_in(own, axis_at), (shards_of,), jnp.float32, smallest / len(cuts), high / len(cuts)))
        gain = gain * jnp.repeat(heights, dims[axis_at] // shards_of).reshape([-1 if axis == axis_at else 1 for axis in range(len(dims))])
    return gain


def noise(own_key, shape, deviation, most, pieces=(), kind=jnp.bfloat16):
    result = deviation * jax.random.normal(own_key, shape, jnp.float32)
    if pieces:
        result = result * levels(own_key, shape, pieces, -0.22, 0.18)
    return jnp.clip(result, -most, most).astype(kind)


def setup_inputs(seed: int = 0) -> dict:
    streams_of = jax.random.split(jax.random.key(seed), 18)
    tokens = draw_tokens(jax.random.fold_in(streams_of[17], 71), 0)
    norm_gain = jnp.clip(1.0 + 0.18 * jax.random.normal(streams_of[1], (LAYERS, D), jnp.float32), 0.1, 1.9)
    w_gate = noise(streams_of[2], (LAYERS, D, SSDW), D ** -0.5, 0.09375, ((2, 32),))
    w_value = noise(streams_of[3], (LAYERS, D, SSDW), D ** -0.5, 0.09375, ((2, 32),))
    w_write = noise(streams_of[4], (LAYERS, D, GROUPS * STATE), D ** -0.5, 0.09375, ((2, 32),))
    w_read = noise(streams_of[5], (LAYERS, D, GROUPS * STATE), D ** -0.5, 0.09375, ((2, 32),))
    w_step = noise(streams_of[6], (LAYERS, D, HEADS), D ** -0.5, 0.09375)
    step_bias = jnp.clip(jax.random.uniform(streams_of[7], (LAYERS, HEADS), jnp.float32, -2.0, 1.0), -2.0, 1.0)
    decay_rate = jnp.clip(jnp.exp(jax.random.uniform(streams_of[8], (LAYERS, HEADS), jnp.float32, math.log(0.05), math.log(3.0))), 0.05, 3.0)
    skip_gain = jnp.clip(jnp.exp(jax.random.uniform(streams_of[9], (LAYERS, HEADS), jnp.float32, math.log(1.0), math.log(4.0))), 1.0, 4.0)
    conv_value_weight = noise(streams_of[10], (LAYERS, CONV, SSDW), 0.577, 2.5, ((2, 32),), jnp.float32)
    conv_key_weight = noise(streams_of[11], (LAYERS, CONV, 2, GROUPS * STATE), 0.577, 2.5, ((3, 32),), jnp.float32)
    group_gain = jnp.clip(1.0 + 0.18 * jax.random.normal(streams_of[12], (LAYERS, SSDW), jnp.float32), 0.1, 1.9)
    w_out = noise(streams_of[13], (LAYERS, SSDW, D), SSDW ** -0.5, 0.0625, ((1, 32),))
    ssm_state = noise(streams_of[14], (LAYERS, BATCH, SSDW, STATE), 0.5, 3.0, ((2, 32),), jnp.float32)
    conv_value = noise(streams_of[15], (LAYERS, BATCH, CONV - 1, SSDW), 1.0, 5.0, ((3, 32),), jnp.float32)
    conv_key = noise(streams_of[16], (LAYERS, BATCH, CONV - 1, 2, GROUPS * STATE), 1.0, 5.0, ((4, 32),), jnp.float32)
    return {"tokens": tokens, "norm_gain": norm_gain, "w_gate": w_gate, "w_value": w_value, "w_write": w_write, "w_read": w_read, "w_step": w_step, "step_bias": step_bias, "decay_rate": decay_rate, "skip_gain": skip_gain, "conv_value_weight": conv_value_weight, "conv_key_weight": conv_key_weight, "group_gain": group_gain, "w_out": w_out, "ssm_state": ssm_state, "conv_value": conv_value, "conv_key": conv_key}


EPS = 1e-06

def reference(tokens, norm_gain, w_gate, w_value, w_write, w_read, w_step, step_bias, decay_rate, skip_gain, conv_value_weight, conv_key_weight, group_gain, w_out, ssm_state, conv_value, conv_key):
    hidden = tokens
    ssm_list = []
    value_list = []
    key_list = []
    for layer in range(LAYERS):
        resid = hidden.astype(jnp.float32)
        inv_scale = lax.rsqrt(lax.optimization_barrier(jnp.sum(resid * resid, axis=1)) / D + EPS)[:, None]
        scaled = (resid * norm_gain[layer]).astype(jnp.bfloat16)

        def project(weight):
            return jnp.dot(scaled, weight[layer], preferred_element_type=jnp.float32) * inv_scale
        gate_in = project(w_gate)
        value_in = project(w_value)
        write_in = project(w_write)
        read_in = project(w_read)
        step_in = project(w_step)
        value_window = jnp.concatenate([conv_value[layer], value_in[:, None, :]], axis=1)
        value_list.append(value_window[:, 1:])
        values = jax.nn.silu(lax.optimization_barrier(jnp.sum(value_window * conv_value_weight[layer][None], axis=1)))
        values = values.reshape(BATCH, GROUPS, HPG, HEAD_DIM)
        fresh = jnp.stack([write_in, read_in], axis=1)[:, None]
        key_window = jnp.concatenate([conv_key[layer], fresh], axis=1)
        key_list.append(key_window[:, 1:])
        mixed_keys = jax.nn.silu(lax.optimization_barrier(jnp.sum(key_window * conv_key_weight[layer][None], axis=1)))
        writes = jnp.transpose(mixed_keys[:, 0].reshape(BATCH, STATE, GROUPS), (0, 2, 1))
        reads = jnp.transpose(mixed_keys[:, 1].reshape(BATCH, STATE, GROUPS), (0, 2, 1))
        delta = jax.nn.softplus(step_in + step_bias[layer][None])
        decay = jnp.exp(-delta * decay_rate[layer][None])
        delta = delta.reshape(BATCH, GROUPS, HPG)
        decay = decay.reshape(BATCH, GROUPS, HPG)
        state = ssm_state[layer].reshape(BATCH, GROUPS, HPG, HEAD_DIM, STATE)
        state = decay[..., None, None] * state + (delta[..., None] * values)[..., None] * writes[:, :, None, None, :]
        ssm_list.append(state.reshape(BATCH, SSDW, STATE))
        read_out = jnp.einsum('bghpn,bgn->bghp', state, reads, precision=lax.Precision.HIGHEST)
        read_out = read_out + skip_gain[layer].reshape(GROUPS, HPG)[None, :, :, None] * values
        gated = read_out.reshape(BATCH, GROUPS, GW) * jax.nn.silu(gate_in.reshape(BATCH, GROUPS, GW))
        group_scale = lax.rsqrt(lax.optimization_barrier(jnp.mean(gated * gated, axis=2, keepdims=True)) + EPS)
        normed = (gated * group_scale * group_gain[layer].reshape(GROUPS, GW)[None]).astype(jnp.bfloat16)
        update = jnp.dot(normed.reshape(BATCH, SSDW), w_out[layer], preferred_element_type=jnp.float32)
        hidden = (resid + update).astype(jnp.bfloat16)
    return (hidden, jnp.stack(ssm_list), jnp.stack(value_list), jnp.stack(key_list))
```

```python
import jax
import jax.numpy as jnp
from jax import lax
from jax.experimental import pallas as pl
from jax.experimental.pallas import tpu as pltpu
from jax.sharding import PartitionSpec as P
import functools

D = 4096
HEAD_DIM = 64
GROUPS = 8
STATE = 128
LAYERS = 2
HEADS = 128
GW = 1024


EPS = 1e-06


def per_device(
    tokens,
    norm_gain,
    w_gate,
    w_value,
    w_write,
    w_read,
    w_step,
    step_bias,
    decay_rate,
    skip_gain,
    conv_value_weight,
    conv_key_weight,
    group_gain,
    w_out,
    ssm_state,
    conv_value,
    conv_key,
):
    highest = lax.Precision.HIGHEST
    chan_count = w_gate.shape[2]
    position = lax.axis_index("tp")
    first_chan = position * chan_count
    chan_ids = first_chan + jnp.arange(chan_count, dtype=jnp.int32)
    my_group = first_chan // GW
    head_hot = (
        (chan_ids // HEAD_DIM)[:, None] == jnp.arange(HEADS, dtype=jnp.int32)[None, :]
    ).astype(jnp.float32)
    group_hot = ((chan_ids // GW)[:, None] == jnp.arange(GROUPS, dtype=jnp.int32)[None, :]).astype(
        jnp.float32
    )
    hidden = tokens
    ssm_list = []
    value_list = []
    key_list = []
    for layer in range(LAYERS):
        resid = hidden.astype(jnp.float32)
        inv_scale = lax.rsqrt(jnp.sum(resid * resid, axis=1) / D + EPS)[:, None]
        scaled = (resid * norm_gain[layer]).astype(jnp.bfloat16)

        def project(weight):
            return jnp.dot(scaled, weight[layer], preferred_element_type=jnp.float32) * inv_scale

        gate_in = project(w_gate)
        value_in = project(w_value)
        write_in = project(w_write)
        read_in = project(w_read)
        step_in = project(w_step)
        value_window = jnp.concatenate([conv_value[layer], value_in[:, None, :]], axis=1)
        value_list.append(value_window[:, 1:])
        values = jax.nn.silu(jnp.sum(value_window * conv_value_weight[layer][None], axis=1))
        fresh = jnp.stack([write_in, read_in], axis=1)[:, None]
        key_window = jnp.concatenate([conv_key[layer], fresh], axis=1)
        key_list.append(key_window[:, 1:])
        mixed_keys = jax.nn.silu(jnp.sum(key_window * conv_key_weight[layer][None], axis=1))
        every_group = lax.all_gather(mixed_keys, "tp", axis=2, tiled=True)
        by_entry = every_group.reshape(every_group.shape[0], 2, STATE, GROUPS)
        own_keys = lax.dynamic_slice_in_dim(by_entry, my_group, 1, 3)[..., 0]
        writes = own_keys[:, 0]
        reads = own_keys[:, 1]
        delta = jax.nn.softplus(step_in + step_bias[layer][None])
        decay = jnp.exp(-delta * decay_rate[layer][None])
        delta_chan = jnp.dot(delta, head_hot.T, precision=highest)
        decay_chan = jnp.dot(decay, head_hot.T, precision=highest)
        skip_chan = jnp.dot(skip_gain[layer], head_hot.T, precision=highest)
        state = (
            decay_chan[..., None] * ssm_state[layer]
            + (delta_chan * values)[..., None] * writes[:, None, :]
        )
        ssm_list.append(state)
        read_out = jnp.sum(state * reads[:, None, :], axis=2) + skip_chan[None] * values
        gated = read_out * jax.nn.silu(gate_in)
        squares = jnp.dot(gated * gated, group_hot, precision=highest)
        square_total = lax.psum(squares, "tp")
        group_scale = lax.rsqrt(square_total / GW + EPS)
        scale_chan = jnp.dot(group_scale, group_hot.T, precision=highest)
        normed = (gated * scale_chan * group_gain[layer][None]).astype(jnp.bfloat16)
        partial_out = jnp.dot(normed, w_out[layer], preferred_element_type=jnp.float32)
        update = lax.psum(partial_out, "tp")
        hidden = (resid + update).astype(jnp.bfloat16)
    return (hidden, jnp.stack(ssm_list), jnp.stack(value_list), jnp.stack(key_list))


LANES = 128
TAPS = 3
BF16 = jnp.bfloat16
F32 = jnp.float32
NT = (((1,), (1,)), ((), ()))


def split3(x):
    high = x.astype(BF16)
    rest = x - high.astype(F32)
    mid = rest.astype(BF16)
    return high, mid, (rest - mid.astype(F32)).astype(BF16)


def select_dot(x, hot):
    rows = x.shape[0]
    parts = jnp.concatenate(split3(x), axis=0)
    out = jnp.dot(parts, hot, preferred_element_type=F32)
    return out[:rows] + out[rows : 2 * rows] + out[2 * rows :]


def silu(v):
    return v / (1.0 + jnp.exp(-v))


def iota(shape, axis):
    return lax.broadcasted_iota(jnp.int32, shape, axis)


def kernel(
    n,
    tokens_hbm,
    gain_hbm,
    wg_hbm,
    wv_hbm,
    ww_hbm,
    wr_hbm,
    ws_hbm,
    bias_hbm,
    rate_hbm,
    skip_hbm,
    cvw_hbm,
    ckw_hbm,
    gg_hbm,
    wo_hbm,
    state_hbm,
    cv_hbm,
    ck_hbm,
    tokens_out,
    state_out,
    value_out,
    write_out,
    read_out_ref,
    tokens,
    gain,
    wg,
    wv,
    ww,
    wr,
    ws,
    bias,
    rate,
    skip,
    cvw,
    ckw,
    gg,
    wo,
    state,
    cv,
    ck,
    hidden,
    scaled,
    keys_send,
    keys_recv,
    sq_send,
    sq_recv,
    part,
    rs_send,
    rs_recv,
    cols,
    wbuf,
    rbuf,
    qbuf,
    in_small,
    in_big,
    out_sem,
    key_ss,
    key_rs,
    sq_ss,
    sq_rs,
    rs_ss,
    rs_rs,
    ag_ss,
    ag_rs,
):
    layers, batch, chans, entries = state.shape
    width = hidden.shape[3]
    depth = tokens.shape[1]
    key_cols = ww.shape[2]
    own_entries = key_cols // GROUPS
    span = 2 * own_entries
    heads = bias.shape[1]
    peers = GW // chans
    me = lax.axis_index("tp")
    my_group = me // peers
    first = my_group * peers
    kstep = 512
    ksteps = depth // kstep

    small_pairs = (
        (tokens_hbm, tokens),
        (gain_hbm, gain),
        (bias_hbm, bias),
        (rate_hbm, rate),
        (skip_hbm, skip),
        (cvw_hbm, cvw),
        (ckw_hbm, ckw),
        (gg_hbm, gg),
        (cv_hbm, cv),
        (ck_hbm, ck),
    )
    small = [pltpu.make_async_copy(a, b, in_small.at[i]) for i, (a, b) in enumerate(small_pairs)]
    big = [
        [
            pltpu.make_async_copy(a.at[l], b.at[l], in_big.at[l, i])
            for i, (a, b) in enumerate(
                (
                    (ww_hbm, ww),
                    (wr_hbm, wr),
                    (wg_hbm, wg),
                    (wv_hbm, wv),
                    (ws_hbm, ws),
                    (state_hbm, state),
                    (wo_hbm, wo),
                )
            )
        ]
        for l in range(layers)
    ]
    for copy in small[:2] + big[0][:2] + small[2:] + big[0][2:] + big[1]:
        copy.start()

    barrier = pltpu.get_barrier_semaphore()

    def greet(k, carry):
        pl.semaphore_signal(
            barrier,
            inc=1,
            device_id=(lax.rem(me + k, n),),
            device_id_type=pl.DeviceIdType.MESH,
        )
        return carry

    lax.fori_loop(1, n, greet, 0)

    def remote(src, dst, ss, rs, to):
        return pltpu.make_async_remote_copy(
            src_ref=src,
            dst_ref=dst,
            send_sem=ss,
            recv_sem=rs,
            device_id=(to,),
            device_id_type=pl.DeviceIdType.MESH,
        )

    def key_copy(l, k, slot):
        to = lax.rem(me + k, n)
        return remote(
            keys_send.at[l, to // peers], keys_recv.at[l, slot], key_ss.at[l, k], key_rs.at[l, k], to
        )

    def rs_copy(l, k, slot):
        to = lax.rem(me + k, n)
        return remote(rs_send.at[l, to], rs_recv.at[l, slot], rs_ss.at[l, k], rs_rs.at[l, k], to)

    def ag_copy(l, k, slot):
        to = lax.rem(me + k, n)
        return remote(
            hidden.at[l, me], hidden.at[l, slot], ag_ss.at[l, k], ag_rs.at[l, k], to
        )

    def sq_copy(l, k):
        to = first + lax.rem(me - first + k, peers)
        return remote(
            sq_send.at[l], sq_recv.at[l, k], sq_ss.at[l, k], sq_rs.at[l, k], to
        )

    def each(body):
        def step(k, carry):
            body(k)
            return carry

        lax.fori_loop(1, n, step, 0)

    def came_from(k):
        return lax.rem(me + n - k, n)

    row = iota((2 * key_cols, key_cols), 0)
    col = iota((2 * key_cols, key_cols), 1)
    source = (row % own_entries) * GROUPS + row // span
    is_read = (row % span) // own_entries
    send_hot = [
        jnp.where((col == source) & (is_read == i), 1.0, 0.0).astype(BF16) for i in range(2)
    ]
    row = iota((n * span, 2 * entries), 0)
    col = iota((n * span, 2 * entries), 1)
    target = ((row % span) // own_entries) * entries + (row // span) * own_entries + row % own_entries
    recv_hot = jnp.where(col == target, 1.0, 0.0).astype(BF16)
    row = iota((heads, chans), 0)
    col = iota((heads, chans), 1)
    head_hot = jnp.where(row == (me * chans + col) // HEAD_DIM, 1.0, 0.0).astype(BF16)

    def update_state(l, group):
        turned = pltpu.roll(cols[...], lax.rem(LANES - 8 * group, LANES), 1)
        writes8 = wbuf[pl.ds(pl.multiple_of(8 * group, 8), 8), :]
        for j in range(8):
            b = 8 * group + j
            state[l, b] = (
                turned[:, batch + j : batch + j + 1] * state[l, b]
                + turned[:, j : j + 1] * writes8[j : j + 1, :]
            )
        pltpu.make_async_copy(
            state.at[l, pl.ds(8 * group, 8)],
            state_out.at[l, pl.ds(8 * group, 8)],
            out_sem.at[l, group],
        ).start()

    groups8 = batch // 8

    def update_range(l, low, high):
        def step(g, carry):
            update_state(l, g)
            return carry

        lax.fori_loop(low, high, step, 0)

    for copy in small[:2]:
        copy.wait()

    for l in range(layers):
        if l == 0:
            def piece(j):
                return tokens[:, j * width : (j + 1) * width]
        else:
            def piece(j):
                return hidden[l - 1, j]
        squares = jnp.zeros((batch, width), F32)
        for j in range(n):
            x = piece(j).astype(F32)
            squares = squares + x * x
            scaled[:, j * width : (j + 1) * width] = (
                x * gain[l : l + 1, j * width : (j + 1) * width]
            ).astype(BF16)
        inv_scale = lax.rsqrt(jnp.sum(squares, axis=1, keepdims=True) / depth + EPS)

        def project(refs):
            def step(k, accs):
                at = pl.ds(pl.multiple_of(k * kstep, kstep), kstep)
                x = scaled[:, at]
                return tuple(
                    acc + jnp.dot(x, ref[l, at, :], preferred_element_type=F32)
                    for acc, ref in zip(accs, refs)
                )

            zeros = tuple(jnp.zeros((batch, ref.shape[2]), F32) for ref in refs)
            return [acc * inv_scale for acc in lax.fori_loop(0, ksteps, step, zeros)]

        big[l][0].wait()
        big[l][1].wait()
        write_in, read_in = project((ww, wr))
        write_out[l] = write_in
        read_out_ref[l] = read_in
        if l == 0:
            for copy in small[2:]:
                copy.wait()
        keys_t = jnp.zeros((2 * key_cols, LANES), F32)
        for i, fresh in enumerate((write_in, read_in)):
            mixed = fresh * ckw[l, TAPS - 1, i : i + 1, :]
            for k in range(TAPS - 1):
                mixed = mixed + ck[l, k, i] * ckw[l, k, i : i + 1, :]
            mixed = jnp.concatenate(
                [silu(mixed), jnp.zeros((LANES - batch, key_cols), F32)], axis=0
            )
            for p in split3(mixed):
                keys_t = keys_t + lax.dot_general(
                    send_hot[i], p, NT, preferred_element_type=F32
                )
        keys_send[l] = keys_t.reshape(GROUPS, span, LANES)
        keys_recv[l, me] = keys_send[l, my_group]
        if l == 0:
            pl.semaphore_wait(barrier, n - 1)
        each(lambda k: key_copy(l, k, me).start())

        big[l][2].wait()
        big[l][3].wait()
        big[l][4].wait()
        gate_in, value_in, step_in = project((wg, wv, ws))
        value_out[l] = value_in
        values = value_in * cvw[l, TAPS - 1 : TAPS, :]
        for k in range(TAPS - 1):
            values = values + cv[l, k] * cvw[l, k : k + 1, :]
        values = silu(values)
        raw = step_in + bias[l : l + 1, :]
        delta = jnp.maximum(raw, 0.0) + jnp.log1p(jnp.exp(-jnp.abs(raw)))
        decay = jnp.exp(-delta * rate[l : l + 1, :])
        skips = jnp.broadcast_to(skip[l : l + 1, :], (8, heads))
        chan = select_dot(jnp.concatenate([delta, decay, skips], axis=0), head_hot)
        decay_chan = chan[batch : 2 * batch]
        skip_chan = chan[2 * batch : 2 * batch + 1]
        dv = chan[:batch] * values
        cols[...] = jnp.concatenate(
            [dv, decay_chan, jnp.zeros((LANES - 2 * batch, chans), F32)], axis=0
        ).T
        gate = silu(gate_in)
        big[l][5].wait()

        each(lambda k: key_copy(l, k, came_from(k)).wait_recv())
        arrived = keys_recv[l].reshape(n * span, LANES).T[:batch]
        both = select_dot(arrived, recv_hot)
        writes = both[:, :entries]
        reads = both[:, entries:]
        wbuf[...] = writes
        rbuf[...] = reads
        lane_half = iota((8, 2 * entries), 1) // entries
        sub = iota((8, 2 * entries), 0)

        def query(g, carry):
            at = pl.ds(pl.multiple_of(8 * g, 8), 8)
            reads8 = rbuf[at, :]
            twice = jnp.concatenate([reads8, reads8], axis=1)
            total = jnp.zeros((8, chans), F32)
            for p in range(4):
                left = jnp.where(sub == 2 * p + lane_half, twice, 0.0).astype(BF16)
                right = jnp.concatenate(
                    [state[l, 8 * g + 2 * p], state[l, 8 * g + 2 * p + 1]], axis=1
                ).astype(BF16)
                total = total + lax.dot_general(left, right, NT, preferred_element_type=F32)
            qbuf[at, :] = total
            return carry

        lax.fori_loop(0, groups8, query, 0)
        through = jnp.sum(writes * reads, axis=1, keepdims=True)
        mixed_out = decay_chan * qbuf[...] + dv * through + skip_chan * values
        gated = mixed_out * gate
        sq_send[l] = jnp.broadcast_to(
            jnp.sum(gated * gated, axis=1, keepdims=True), (batch, LANES)
        )
        for k in range(1, peers):
            sq_copy(l, k).start()
        fed = (gated * gg[l : l + 1, :]).astype(BF16)
        big[l][6].wait()
        per = 4

        def out_step(t, carry):
            res = jnp.dot(
                fed,
                wo[l, :, pl.ds(pl.multiple_of(t * per * width, per * width), per * width)],
                preferred_element_type=F32,
            )
            for i in range(per):
                part[t * per + i] = res[:, i * width : (i + 1) * width]
            return carry

        lax.fori_loop(0, n // per, out_step, 0)
        for k in range(1, peers):
            sq_copy(l, k).wait_recv()
        total = sq_send[l]
        for k in range(1, peers):
            total = total + sq_recv[l, k]
        scale = lax.rsqrt(total / GW + EPS)
        for j in range(n):
            rs_send[l, j] = (part[j] * scale[:, :width]).astype(BF16)
        each(lambda k: rs_copy(l, k, me).start())
        update_range(l, 0, groups8 // 2)
        own = part[me] * scale[:, :width]
        if l == 0:
            resid = tokens[:, pl.ds(pl.multiple_of(me * width, width), width)]
        else:
            resid = hidden[l - 1, me]
        each(lambda k: rs_copy(l, k, came_from(k)).wait_recv())
        rs_recv[l, me] = jnp.zeros((batch, width), BF16)
        sums = [own, jnp.zeros_like(own), jnp.zeros_like(own), jnp.zeros_like(own)]
        for j in range(n):
            sums[j % 4] = sums[j % 4] + rs_recv[l, j].astype(F32)
        update = (sums[0] + sums[1]) + (sums[2] + sums[3])
        hidden[l, me] = (resid.astype(F32) + update).astype(BF16)
        each(lambda k: ag_copy(l, k, me).start())
        update_range(l, groups8 // 2, groups8)
        each(lambda k: ag_copy(l, k, came_from(k)).wait_recv())

    for j in range(n):
        tokens_out[:, j * width : (j + 1) * width] = hidden[layers - 1, j]
    for l in range(layers):
        def drain(k):
            key_copy(l, k, me).wait_send()
            rs_copy(l, k, me).wait_send()
            ag_copy(l, k, me).wait_send()

        each(drain)
        for k in range(1, peers):
            sq_copy(l, k).wait_send()
        for g in range(groups8):
            pltpu.make_async_copy(
                state.at[l, pl.ds(8 * g, 8)],
                state_out.at[l, pl.ds(8 * g, 8)],
                out_sem.at[l, g],
            ).wait()


def fused(n, *args):
    (tokens, norm_gain, w_gate, w_value, w_write, w_read, w_step, step_bias, decay_rate) = args[:9]
    (skip_gain, cvw, ckw, group_gain, w_out, ssm_state, conv_value, conv_key) = args[9:]
    layers, batch, chans, entries = ssm_state.shape
    depth = tokens.shape[1]
    key_cols = w_write.shape[2]
    peers = GW // chans
    span = 2 * (key_cols // GROUPS)
    width = depth // n
    operands = list(args[:15]) + [
        jnp.transpose(conv_value, (0, 2, 1, 3)),
        jnp.transpose(conv_key, (0, 2, 3, 1, 4)),
    ]
    landed = [pltpu.VMEM(a.shape, a.dtype) for a in operands]
    dma = pltpu.SemaphoreType.DMA
    hidden, state, value_in, write_in, read_in = pl.pallas_call(
        functools.partial(kernel, n),
        out_shape=(
            jax.ShapeDtypeStruct(tokens.shape, BF16),
            jax.ShapeDtypeStruct(ssm_state.shape, F32),
            jax.ShapeDtypeStruct((layers, batch, chans), F32),
            jax.ShapeDtypeStruct((layers, batch, key_cols), F32),
            jax.ShapeDtypeStruct((layers, batch, key_cols), F32),
        ),
        in_specs=[pl.BlockSpec(memory_space=pl.ANY)] * len(operands),
        out_specs=(
            pl.BlockSpec(memory_space=pltpu.VMEM),
            pl.BlockSpec(memory_space=pl.ANY),
            pl.BlockSpec(memory_space=pltpu.VMEM),
            pl.BlockSpec(memory_space=pltpu.VMEM),
            pl.BlockSpec(memory_space=pltpu.VMEM),
        ),
        scratch_shapes=landed
        + [
            pltpu.VMEM((layers, n, batch, width), BF16),
            pltpu.VMEM((batch, depth), BF16),
            pltpu.VMEM((layers, GROUPS, span, LANES), F32),
            pltpu.VMEM((layers, n, span, LANES), F32),
            pltpu.VMEM((layers, batch, LANES), F32),
            pltpu.VMEM((layers, peers, batch, LANES), F32),
            pltpu.VMEM((n, batch, width), F32),
            pltpu.VMEM((layers, n, batch, width), BF16),
            pltpu.VMEM((layers, n, batch, width), BF16),
            pltpu.VMEM((chans, LANES), F32),
            pltpu.VMEM((batch, entries), F32),
            pltpu.VMEM((batch, entries), F32),
            pltpu.VMEM((batch, chans), F32),
            dma((10,)),
            dma((layers, 7)),
            dma((layers, batch // 8)),
            dma((layers, n)),
            dma((layers, n)),
            dma((layers, peers)),
            dma((layers, peers)),
            dma((layers, n)),
            dma((layers, n)),
            dma((layers, n)),
            dma((layers, n)),
        ],
        compiler_params=pltpu.CompilerParams(
            collective_id=0, has_side_effects=True, vmem_limit_bytes=60 * 1024 * 1024
        ),
        name="mixer",
    )(*operands)
    value_state = jnp.concatenate([conv_value[:, :, 1:], value_in[:, :, None]], axis=2)
    fresh = jnp.stack([write_in, read_in], axis=2)[:, :, None]
    key_state = jnp.concatenate([conv_key[:, :, 1:], fresh], axis=2)
    return hidden, state, value_state, key_state


def dispatch(n, *args):
    depth = args[0].shape[1]
    batch, chans = args[14].shape[1:3]
    own_entries = args[4].shape[2] // GROUPS
    fits = (
        depth == n * LANES
        and 2 * own_entries == 8
        and chans % LANES == 0
        and GW % chans == 0
        and 2 * batch <= LANES
        and batch % 16 == 0
    )
    return fused(n, *args) if fits else per_device(*args)


def solution(mesh):
    placed = (
        P(),
        P(),
        P(None, None, "tp"),
        P(None, None, "tp"),
        P(None, None, "tp"),
        P(None, None, "tp"),
        P(),
        P(),
        P(),
        P(),
        P(None, None, "tp"),
        P(None, None, None, "tp"),
        P(None, "tp"),
        P(None, "tp", None),
        P(None, None, "tp", None),
        P(None, None, None, "tp"),
        P(None, None, None, None, "tp"),
    )
    return jax.shard_map(
        functools.partial(dispatch, mesh.shape["tp"]),
        mesh=mesh,
        in_specs=placed,
        out_specs=(
            P(),
            P(None, None, "tp", None),
            P(None, None, None, "tp"),
            P(None, None, None, None, "tp"),
        ),
        check_vma=False,
    )
```

```python
import jax
import jax.numpy as jnp
from jax import lax
from jax.experimental import pallas as pl
from jax.experimental.pallas import tpu as pltpu
from jax.sharding import PartitionSpec as P
import functools

D = 4096
HEAD_DIM = 64
GROUPS = 8
STATE = 128
LAYERS = 2
HEADS = 128
GW = 1024


EPS = 1e-06


def per_device(
    tokens,
    norm_gain,
    w_gate,
    w_value,
    w_write,
    w_read,
    w_step,
    step_bias,
    decay_rate,
    skip_gain,
    conv_value_weight,
    conv_key_weight,
    group_gain,
    w_out,
    ssm_state,
    conv_value,
    conv_key,
):
    highest = lax.Precision.HIGHEST
    chan_count = w_gate.shape[2]
    position = lax.axis_index("tp")
    first_chan = position * chan_count
    chan_ids = first_chan + jnp.arange(chan_count, dtype=jnp.int32)
    my_group = first_chan // GW
    head_hot = (
        (chan_ids // HEAD_DIM)[:, None] == jnp.arange(HEADS, dtype=jnp.int32)[None, :]
    ).astype(jnp.float32)
    group_hot = ((chan_ids // GW)[:, None] == jnp.arange(GROUPS, dtype=jnp.int32)[None, :]).astype(
        jnp.float32
    )
    hidden = tokens
    ssm_list = []
    value_list = []
    key_list = []
    for layer in range(LAYERS):
        resid = hidden.astype(jnp.float32)
        inv_scale = lax.rsqrt(jnp.sum(resid * resid, axis=1) / D + EPS)[:, None]
        scaled = (resid * norm_gain[layer]).astype(jnp.bfloat16)

        def project(weight):
            return jnp.dot(scaled, weight[layer], preferred_element_type=jnp.float32) * inv_scale

        gate_in = project(w_gate)
        value_in = project(w_value)
        write_in = project(w_write)
        read_in = project(w_read)
        step_in = project(w_step)
        value_window = jnp.concatenate([conv_value[layer], value_in[:, None, :]], axis=1)
        value_list.append(value_window[:, 1:])
        values = jax.nn.silu(jnp.sum(value_window * conv_value_weight[layer][None], axis=1))
        fresh = jnp.stack([write_in, read_in], axis=1)[:, None]
        key_window = jnp.concatenate([conv_key[layer], fresh], axis=1)
        key_list.append(key_window[:, 1:])
        mixed_keys = jax.nn.silu(jnp.sum(key_window * conv_key_weight[layer][None], axis=1))
        every_group = lax.all_gather(mixed_keys, "tp", axis=2, tiled=True)
        by_entry = every_group.reshape(every_group.shape[0], 2, STATE, GROUPS)
        own_keys = lax.dynamic_slice_in_dim(by_entry, my_group, 1, 3)[..., 0]
        writes = own_keys[:, 0]
        reads = own_keys[:, 1]
        delta = jax.nn.softplus(step_in + step_bias[layer][None])
        decay = jnp.exp(-delta * decay_rate[layer][None])
        delta_chan = jnp.dot(delta, head_hot.T, precision=highest)
        decay_chan = jnp.dot(decay, head_hot.T, precision=highest)
        skip_chan = jnp.dot(skip_gain[layer], head_hot.T, precision=highest)
        state = (
            decay_chan[..., None] * ssm_state[layer]
            + (delta_chan * values)[..., None] * writes[:, None, :]
        )
        ssm_list.append(state)
        read_out = jnp.sum(state * reads[:, None, :], axis=2) + skip_chan[None] * values
        gated = read_out * jax.nn.silu(gate_in)
        squares = jnp.dot(gated * gated, group_hot, precision=highest)
        square_total = lax.psum(squares, "tp")
        group_scale = lax.rsqrt(square_total / GW + EPS)
        scale_chan = jnp.dot(group_scale, group_hot.T, precision=highest)
        normed = (gated * scale_chan * group_gain[layer][None]).astype(jnp.bfloat16)
        partial_out = jnp.dot(normed, w_out[layer], preferred_element_type=jnp.float32)
        update = lax.psum(partial_out, "tp")
        hidden = (resid + update).astype(jnp.bfloat16)
    return (hidden, jnp.stack(ssm_list), jnp.stack(value_list), jnp.stack(key_list))


LANES = 128
TAPS = 3
VMEM = 67043328
BF16 = jnp.bfloat16
F32 = jnp.float32
NT = (((1,), (1,)), ((), ()))


def split3(x):
    high = x.astype(BF16)
    rest = x - high.astype(F32)
    mid = rest.astype(BF16)
    return high, mid, (rest - mid.astype(F32)).astype(BF16)


def select_dot(x, hot):
    rows = x.shape[0]
    parts = jnp.concatenate(split3(x), axis=0)
    out = jnp.dot(parts, hot, preferred_element_type=F32)
    return out[:rows] + out[rows : 2 * rows] + out[2 * rows :]


def silu(v):
    return v / (1.0 + jnp.exp(-v))


def iota(shape, axis):
    return lax.broadcasted_iota(jnp.int32, shape, axis)


def kernel(
    n,
    tokens_hbm,
    gain_hbm,
    wg_hbm,
    wv_hbm,
    ww_hbm,
    wr_hbm,
    ws_hbm,
    bias_hbm,
    rate_hbm,
    skip_hbm,
    cvw_hbm,
    ckw_hbm,
    gg_hbm,
    wo_hbm,
    state_hbm,
    cv_hbm,
    ck_hbm,
    tokens_out,
    state,
    value_out,
    key_out,
    tokens,
    gain,
    wg,
    wv,
    wk,
    ws,
    bias,
    rate,
    skip,
    cvw,
    ckw,
    gg,
    wo,
    cv,
    ck,
    hidden,
    scaled,
    keys_send,
    keys_recv,
    sq_send,
    sq_recv,
    part,
    rs_send,
    rs_recv,
    cols,
    wbuf,
    rbuf,
    qbuf,
    in_small,
    in_big,
    key_ss,
    key_rs,
    sq_ss,
    sq_rs,
    rs_ss,
    rs_rs,
    ag_ss,
    ag_rs,
):
    layers, batch, chans, entries = state.shape
    width = hidden.shape[3]
    depth = tokens.shape[1]
    key_cols = wk.shape[1] // 2
    own_entries = key_cols // GROUPS
    span = 2 * own_entries
    heads = bias.shape[1]
    peers = GW // chans
    me = lax.axis_index("tp")
    my_group = me // peers
    first = my_group * peers
    kstep = 512
    ksteps = depth // kstep

    small_pairs = (
        (tokens_hbm, tokens),
        (gain_hbm, gain),
        (bias_hbm, bias),
        (rate_hbm, rate),
        (skip_hbm, skip),
        (cvw_hbm, cvw),
        (ckw_hbm, ckw),
        (gg_hbm, gg),
        (cv_hbm, cv),
        (ck_hbm, ck),
    )
    small = [pltpu.make_async_copy(a, b, in_small.at[i]) for i, (a, b) in enumerate(small_pairs)]
    big = [
        [
            pltpu.make_async_copy(a.at[l], b.at[l], in_big.at[l, i])
            for i, (a, b) in enumerate(
                (
                    (ww_hbm, wk.at[:, :key_cols]),
                    (wr_hbm, wk.at[:, key_cols:]),
                    (wg_hbm, wg),
                    (wv_hbm, wv),
                    (ws_hbm, ws),
                    (state_hbm, state),
                    (wo_hbm, wo),
                )
            )
        ]
        for l in range(layers)
    ]
    for copy in small[:2] + big[0][:2] + small[2:] + big[0][2:] + big[1]:
        copy.start()

    barrier = pltpu.get_barrier_semaphore()

    def greet(k, carry):
        pl.semaphore_signal(
            barrier,
            inc=1,
            device_id=(lax.rem(me + k, n),),
            device_id_type=pl.DeviceIdType.MESH,
        )
        return carry

    lax.fori_loop(1, n, greet, 0)

    def remote(src, dst, ss, rs, to):
        return pltpu.make_async_remote_copy(
            src_ref=src,
            dst_ref=dst,
            send_sem=ss,
            recv_sem=rs,
            device_id=(to,),
            device_id_type=pl.DeviceIdType.MESH,
        )

    def key_copy(l, k, slot):
        to = lax.rem(me + k, n)
        return remote(
            keys_send.at[l, to // peers], keys_recv.at[l, slot], key_ss.at[l, k], key_rs.at[l, k], to
        )

    def rs_copy(l, k, slot):
        to = lax.rem(me + k, n)
        return remote(rs_send.at[l, to], rs_recv.at[l, slot], rs_ss.at[l, k], rs_rs.at[l, k], to)

    def ag_copy(l, k, slot):
        to = lax.rem(me + k, n)
        return remote(
            hidden.at[l, me], hidden.at[l, slot], ag_ss.at[l, k], ag_rs.at[l, k], to
        )

    buddy = me + 1 - 2 * lax.rem(me, 2)

    def pair_copy(l, k, slot):
        return remote(
            hidden.at[l, slot], hidden.at[l, slot], ag_ss.at[l, k], ag_rs.at[l, k], buddy
        )

    def sq_copy(l, k):
        to = first + lax.rem(me - first + k, peers)
        return remote(
            sq_send.at[l], sq_recv.at[l, k], sq_ss.at[l, k], sq_rs.at[l, k], to
        )

    def each(body):
        def step(k, carry):
            body(k)
            return carry

        lax.fori_loop(1, n, step, 0)

    def halves(body):
        def step(k, carry):
            body(2 * k)
            return carry

        lax.fori_loop(1, n // 2, step, 0)

    def came_from(k):
        return lax.rem(me + n - k, n)

    row = iota((2 * key_cols, key_cols), 0)
    col = iota((2 * key_cols, key_cols), 1)
    source = (row % own_entries) * GROUPS + row // span
    is_read = (row % span) // own_entries
    send_hot = [
        jnp.where((col == source) & (is_read == i), 1.0, 0.0).astype(BF16) for i in range(2)
    ]
    row = iota((n * span, 2 * entries), 0)
    col = iota((n * span, 2 * entries), 1)
    target = ((row % span) // own_entries) * entries + (row // span) * own_entries + row % own_entries
    recv_hot = jnp.where(col == target, 1.0, 0.0).astype(BF16)
    row = iota((heads, chans), 0)
    col = iota((heads, chans), 1)
    head_hot = jnp.where(row == (me * chans + col) // HEAD_DIM, 1.0, 0.0).astype(BF16)

    def update_state(l, group):
        turned = pltpu.roll(cols[...], lax.rem(LANES - 8 * group, LANES), 1)
        writes8 = wbuf[pl.ds(pl.multiple_of(8 * group, 8), 8), :]
        for j in range(8):
            b = 8 * group + j
            state[l, b] = (
                turned[:, batch + j : batch + j + 1] * state[l, b]
                + turned[:, j : j + 1] * writes8[j : j + 1, :]
            )

    groups8 = batch // 8

    def update_range(l, low, high):
        def step(g, carry):
            update_state(l, g)
            return carry

        lax.fori_loop(low, high, step, 0)

    for copy in small[:2]:
        copy.wait()

    for l in range(layers):
        if l == 0:
            def piece(j):
                return tokens[:, j * width : (j + 1) * width]
        else:
            def piece(j):
                return hidden[l - 1, j]
        squares = jnp.zeros((batch, width), F32)
        for j in range(n):
            x = piece(j).astype(F32)
            squares = squares + x * x
            scaled[:, j * width : (j + 1) * width] = (
                x * gain[l : l + 1, j * width : (j + 1) * width]
            ).astype(BF16)
        inv_scale = lax.rsqrt(jnp.sum(squares, axis=1, keepdims=True) / depth + EPS)

        def project(refs):
            def step(k, accs):
                at = pl.ds(pl.multiple_of(k * kstep, kstep), kstep)
                x = scaled[:, at]
                return tuple(
                    acc + jnp.dot(x, ref[l, at, :], preferred_element_type=F32)
                    for acc, ref in zip(accs, refs)
                )

            zeros = tuple(jnp.zeros((batch, ref.shape[2]), F32) for ref in refs)
            return [acc * inv_scale for acc in lax.fori_loop(0, ksteps, step, zeros)]

        big[l][0].wait()
        big[l][1].wait()
        def key_step(k, acc):
            at = pl.ds(pl.multiple_of(k * kstep, kstep), kstep)
            return acc + lax.dot_general(
                scaled[:, at], wk[l, :, at], NT, preferred_element_type=F32
            )

        key_in = lax.fori_loop(0, ksteps, key_step, jnp.zeros((batch, 2 * key_cols), F32))
        key_in = key_in * inv_scale
        write_in = key_in[:, :key_cols]
        read_in = key_in[:, key_cols:]
        if l == 0:
            for copy in small[2:]:
                copy.wait()
        for i, fresh in enumerate((write_in, read_in)):
            for k in range(1, TAPS - 1):
                key_out[l, :, k - 1, i, :] = ck[l, :, k, i, :]
            key_out[l, :, TAPS - 2, i, :] = fresh
        keys_t = jnp.zeros((2 * key_cols, LANES), F32)
        for i, fresh in enumerate((write_in, read_in)):
            mixed = fresh * ckw[l, TAPS - 1, i : i + 1, :]
            for k in range(TAPS - 1):
                mixed = mixed + ck[l, :, k, i, :] * ckw[l, k, i : i + 1, :]
            mixed = jnp.concatenate(
                [silu(mixed), jnp.zeros((LANES - batch, key_cols), F32)], axis=0
            )
            for p in split3(mixed):
                keys_t = keys_t + lax.dot_general(
                    send_hot[i], p, NT, preferred_element_type=F32
                )
        keys_send[l] = keys_t.reshape(GROUPS, span, LANES)
        keys_recv[l, me] = keys_send[l, my_group]
        if l == 0:
            pl.semaphore_wait(barrier, n - 1)
        each(lambda k: key_copy(l, k, me).start())

        big[l][2].wait()
        big[l][3].wait()
        big[l][4].wait()
        gate_in, value_in, step_in = project((wg, wv, ws))
        for k in range(1, TAPS - 1):
            value_out[l, :, k - 1, :] = cv[l, :, k, :]
        value_out[l, :, TAPS - 2, :] = value_in
        values = value_in * cvw[TAPS - 1, l : l + 1, :]
        for k in range(TAPS - 1):
            values = values + cv[l, :, k, :] * cvw[k, l : l + 1, :]
        values = silu(values)
        raw = step_in + bias[l : l + 1, :]
        delta = jnp.maximum(raw, 0.0) + jnp.log1p(jnp.exp(-jnp.abs(raw)))
        decay = jnp.exp(-delta * rate[l : l + 1, :])
        skips = jnp.broadcast_to(skip[l : l + 1, :], (8, heads))
        chan = select_dot(jnp.concatenate([delta, decay, skips], axis=0), head_hot)
        decay_chan = chan[batch : 2 * batch]
        skip_chan = chan[2 * batch : 2 * batch + 1]
        dv = chan[:batch] * values
        cols[...] = jnp.concatenate(
            [dv, decay_chan, jnp.zeros((LANES - 2 * batch, chans), F32)], axis=0
        ).T
        gate = silu(gate_in)
        big[l][5].wait()

        each(lambda k: key_copy(l, k, came_from(k)).wait_recv())
        arrived = keys_recv[l].reshape(n * span, LANES).T[:batch]
        both = select_dot(arrived, recv_hot)
        writes = both[:, :entries]
        reads = both[:, entries:]
        wbuf[...] = writes
        rbuf[...] = reads
        lane_half = iota((8, 2 * entries), 1) // entries
        sub = iota((8, 2 * entries), 0)

        def query(g, carry):
            at = pl.ds(pl.multiple_of(8 * g, 8), 8)
            reads8 = rbuf[at, :]
            twice = jnp.concatenate([reads8, reads8], axis=1)
            total = jnp.zeros((8, chans), F32)
            for p in range(4):
                left = jnp.where(sub == 2 * p + lane_half, twice, 0.0).astype(BF16)
                right = jnp.concatenate(
                    [state[l, 8 * g + 2 * p], state[l, 8 * g + 2 * p + 1]], axis=1
                ).astype(BF16)
                total = total + lax.dot_general(left, right, NT, preferred_element_type=F32)
            qbuf[at, :] = total
            return carry

        lax.fori_loop(0, groups8, query, 0)
        through = jnp.sum(writes * reads, axis=1, keepdims=True)
        mixed_out = decay_chan * qbuf[...] + dv * through + skip_chan * values
        gated = mixed_out * gate
        sq_send[l] = jnp.broadcast_to(
            jnp.sum(gated * gated, axis=1, keepdims=True), (batch, LANES)
        )
        for k in range(1, peers):
            sq_copy(l, k).start()
        fed = (gated * gg[l : l + 1, :]).astype(BF16)
        big[l][6].wait()
        per = 4

        def out_step(t, carry):
            res = jnp.dot(
                fed,
                wo[l, :, pl.ds(pl.multiple_of(t * per * width, per * width), per * width)],
                preferred_element_type=F32,
            )
            for i in range(per):
                part[t * per + i] = res[:, i * width : (i + 1) * width]
            return carry

        lax.fori_loop(0, n // per, out_step, 0)
        for k in range(1, peers):
            sq_copy(l, k).wait_recv()
        total = sq_send[l]
        for k in range(1, peers):
            total = total + sq_recv[l, k]
        scale = lax.rsqrt(total / GW + EPS)
        for j in range(n):
            rs_send[l, j] = (part[j] * scale[:, :width]).astype(BF16)
        each(lambda k: rs_copy(l, k, me).start())
        update_range(l, 0, groups8 // 2)
        own = part[me] * scale[:, :width]
        if l == 0:
            resid = tokens[:, pl.ds(pl.multiple_of(me * width, width), width)]
        else:
            resid = hidden[l - 1, me]
        each(lambda k: rs_copy(l, k, came_from(k)).wait_recv())
        rs_recv[l, me] = jnp.zeros((batch, width), BF16)
        sums = [own, jnp.zeros_like(own), jnp.zeros_like(own), jnp.zeros_like(own)]
        for j in range(n):
            sums[j % 4] = sums[j % 4] + rs_recv[l, j].astype(F32)
        update = (sums[0] + sums[1]) + (sums[2] + sums[3])
        hidden[l, me] = (resid.astype(F32) + update).astype(BF16)
        pair_copy(l, 1, me).start()
        halves(lambda k: ag_copy(l, k, me).start())
        update_range(l, groups8 // 2, groups8)

        def forward(k):
            ag_copy(l, k, came_from(k)).wait_recv()
            pair_copy(l, k + 1, came_from(k)).start()

        halves(forward)
        pair_copy(l, 1, buddy).wait_recv()
        halves(lambda k: pair_copy(l, k + 1, lax.rem(buddy + n - k, n)).wait_recv())

    for j in range(n):
        tokens_out[:, j * width : (j + 1) * width] = hidden[layers - 1, j]
    for l in range(layers):
        def drain(k):
            key_copy(l, k, me).wait_send()
            rs_copy(l, k, me).wait_send()

        each(drain)
        pair_copy(l, 1, me).wait_send()

        def drain_pair(k):
            ag_copy(l, k, me).wait_send()
            pair_copy(l, k + 1, came_from(k)).wait_send()

        halves(drain_pair)
        for k in range(1, peers):
            sq_copy(l, k).wait_send()


def fused(n, *args):
    (tokens, norm_gain, w_gate, w_value, w_write, w_read, w_step, step_bias, decay_rate) = args[:9]
    (skip_gain, cvw, ckw, group_gain, w_out, ssm_state, conv_value, conv_key) = args[9:]
    layers, batch, chans, entries = ssm_state.shape
    depth = tokens.shape[1]
    key_cols = w_write.shape[2]
    peers = GW // chans
    span = 2 * (key_cols // GROUPS)
    width = depth // n
    operands = list(args)
    operands[4] = jnp.swapaxes(w_write, 1, 2)
    operands[5] = jnp.swapaxes(w_read, 1, 2)
    operands[10] = jnp.swapaxes(cvw, 0, 1)
    landed = [pltpu.VMEM(a.shape, a.dtype) for a in operands]
    landed[4:6] = [pltpu.VMEM((layers, 2 * key_cols, depth), BF16)]
    del landed[13]
    dma = pltpu.SemaphoreType.DMA
    hidden, state, value_state, key_state = pl.pallas_call(
        functools.partial(kernel, n),
        out_shape=(
            jax.ShapeDtypeStruct(tokens.shape, BF16),
            pltpu.VMEM(ssm_state.shape, F32),
            jax.ShapeDtypeStruct(conv_value.shape, F32),
            jax.ShapeDtypeStruct(conv_key.shape, F32),
        ),
        in_specs=[pl.BlockSpec(memory_space=pltpu.HBM)] * len(operands),
        out_specs=(
            pl.BlockSpec(memory_space=pltpu.VMEM),
            pl.BlockSpec(memory_space=pltpu.VMEM),
            pl.BlockSpec(memory_space=pltpu.VMEM),
            pl.BlockSpec(memory_space=pltpu.VMEM),
        ),
        scratch_shapes=landed
        + [
            pltpu.VMEM((layers, n, batch, width), BF16),
            pltpu.VMEM((batch, depth), BF16),
            pltpu.VMEM((layers, GROUPS, span, LANES), F32),
            pltpu.VMEM((layers, n, span, LANES), F32),
            pltpu.VMEM((layers, batch, LANES), F32),
            pltpu.VMEM((layers, peers, batch, LANES), F32),
            pltpu.VMEM((n, batch, width), F32),
            pltpu.VMEM((layers, n, batch, width), BF16),
            pltpu.VMEM((layers, n, batch, width), BF16),
            pltpu.VMEM((chans, LANES), F32),
            pltpu.VMEM((batch, entries), F32),
            pltpu.VMEM((batch, entries), F32),
            pltpu.VMEM((batch, chans), F32),
            dma((10,)),
            dma((layers, 7)),
            dma((layers, n)),
            dma((layers, n)),
            dma((layers, peers)),
            dma((layers, peers)),
            dma((layers, n)),
            dma((layers, n)),
            dma((layers, n)),
            dma((layers, n)),
        ],
        compiler_params=pltpu.CompilerParams(
            collective_id=0, has_side_effects=True, vmem_limit_bytes=VMEM - ssm_state.size * 4 - 768 * 1024
        ),
        name="mixer",
    )(*operands)
    return hidden, state, value_state, key_state


def dispatch(n, *args):
    depth = args[0].shape[1]
    batch, chans = args[14].shape[1:3]
    own_entries = args[4].shape[2] // GROUPS
    fits = (
        depth == n * LANES
        and 2 * own_entries == 8
        and chans % LANES == 0
        and GW % chans == 0
        and 2 * batch <= LANES
        and batch % 16 == 0
        and n % 2 == 0
    )
    return fused(n, *args) if fits else per_device(*args)


def solution(mesh):
    placed = (
        P(),
        P(),
        P(None, None, "tp"),
        P(None, None, "tp"),
        P(None, None, "tp"),
        P(None, None, "tp"),
        P(),
        P(),
        P(),
        P(),
        P(None, None, "tp"),
        P(None, None, None, "tp"),
        P(None, "tp"),
        P(None, "tp", None),
        P(None, None, "tp", None),
        P(None, None, None, "tp"),
        P(None, None, None, None, "tp"),
    )
    return jax.shard_map(
        functools.partial(dispatch, mesh.shape["tp"]),
        mesh=mesh,
        in_specs=placed,
        out_specs=(
            P(),
            P(None, None, "tp", None),
            P(None, None, None, "tp"),
            P(None, None, None, None, "tp"),
        ),
        check_vma=False,
    )
```
